32 devices in a mesh: ep: 8 (over z, x), tp: 4 (over y, core).
Axes of the slice: x: 2, y: 2, z: 4, core: 2. Of those that a mesh axis runs over, the one named last changes fastest.
Arguments:
- tokens: bfloat16 [1024, 4096], P('ep', 'tp'), may hold values from -6 to 6
- norm_gain: float32 [4096], replicated, may hold values from 0.1 to 1.9
- expert_ids: int32 [1024, 2], P('ep'), may hold values from 0 to 7, all different within a row; in each aligned block of 128 rows (0 to 127, 128 to 255, ...) at most 48 rows name the same one
- expert_gates: float32 [1024, 2], P('ep'), may hold values from 0.2 to 1
- gate_proj: bfloat16 [8, 4096, 512], P('ep', None, 'tp'), may hold values from -0.09375 to 0.09375
- up_proj: bfloat16 [8, 4096, 512], P('ep', None, 'tp'), may hold values from -0.09375 to 0.09375
- down_proj: bfloat16 [8, 512, 4096], P('ep', None, 'tp'), may hold values from -0.25 to 0.25
- shared_gate: bfloat16 [4096, 512], P('ep', 'tp'), may hold values from -0.09375 to 0.09375
- shared_up: bfloat16 [4096, 512], P('ep', 'tp'), may hold values from -0.09375 to 0.09375
- shared_down: bfloat16 [512, 4096], P(None, 'tp'), may hold values from -0.25 to 0.25
Outputs:
- mixed: bfloat16 [1024, 4096], P('ep', 'tp')
The draws below stay inside these ranges and needn't reach their ends.
Inputs may be any that keep to these rules, and one draw needn't show every extreme that they name: `expert_ids`: each row names 2 distinct experts. Among the 128 rows of one index of ep (aligned blocks) no expert is named by more than 48 rows, a bound that some block reaches.
All inputs are finite; a program needn't handle non-finite values.
Results may differ from the reference program's by a relative error of at most 0.0067.
Values may be sent and summed in bfloat16 or wider, within the bound.
No kernel may reach another device: no remote copies, remote signals or barrier semaphores. Data moves between devices by JAX's collectives and lax.ppermute only.
A program may use at most 64 MiB of HBM per device.

```python
import math
import jax
import jax.numpy as jnp
import numpy as np
from jax import lax

D = 4096
EXPERT_DIM = 512
SHARED = 512
TOP = 2
TOK_DEV = 128
EXPERTS = 8
CAP = 48
TOKENS = 1024
N_EP = 8


def block_scale(stream_key, shape, shards, least, high):
    level = 1.0
    for axis_at, shards_of in shards:
        draws = jax.random.uniform(jax.random.fold_in(jax.random.fold_in(stream_key, 6), axis_at), (shards_of,), jnp.float32, least / len(shards), high / len(shards))
        level = level * jnp.repeat(jnp.exp(draws), shape[axis_at] // shards_of).reshape((-1,) + (1,) * (len(shape) - 1 - axis_at))
    return level


def routed_block(stream_key, own, number, rows, number_of, top, bound, lean):
    order = jax.random.permutation(stream_key, number_of)
    packed, usual = portions_of(number_of, rows * top, bound, lean, True), portions_of(number_of, rows * top, bound, lean, False)
    places = jnp.arange(number_of)

    def named(lengths, turn):
        used = int((lengths > 0).sum())
        fixed = max(1, used // 4)
        shifted = fixed + (places - fixed + turn * (used - fixed)) % max(1, number_of - fixed)
        return jnp.zeros((number_of,), jnp.int32).at[order[jnp.where(places < fixed, places, shifted)]].set(jnp.asarray(lengths, jnp.int32))

    lengths = jnp.where(number % 4 == 0, named(packed, number // 4), named(usual, number - number // 4 - 1))
    mixed = jax.random.permutation(jax.random.fold_in(own, 3), number_of)
    source_of, taker = mixed[0:number_of // 2 * 2:2], mixed[1:number_of // 2 * 2:2]
    room = jnp.minimum(lengths[source_of] - 1, bound - lengths[taker]) // 2
    room = jnp.where((source_of == order[0]) | (taker == order[0]) | (lengths[taker] == 0), 0, jnp.maximum(room, 0))
    shifted = jax.random.randint(jax.random.fold_in(own, 4), (number_of // 2,), 0, 1 << 20) % (room + 1)
    lengths = lengths.at[source_of].add(-shifted).at[taker].add(shifted)
    items = jnp.searchsorted(jnp.cumsum(lengths), jnp.arange(rows * top), side="right").astype(jnp.int32)
    listing = items.reshape(top, rows).T
    listing = listing[jax.random.permutation(jax.random.fold_in(own, 1), rows)]
    turn = jax.random.randint(jax.random.fold_in(own, 2), (rows, 1), 0, top)
    return jnp.take_along_axis(listing, (jnp.arange(top)[None, :] + turn) % top, axis=1)


def portions_of(amount, total, bound, slope, full):
    weights = [(1 << 20) // math.isqrt(rank ** slope) + 1 for rank in range(1, amount + 1)]
    largest = bound if full else min(bound, max(-(-total // amount), total * weights[0] // sum(weights)))
    least = 1 if total - largest >= amount - 1 else 0
    given, rest = [largest] + [least] * (amount - 1), total - largest - least * (amount - 1)
    while rest > 0:
        movable = [i for i in range(1, amount) if given[i] < largest] or [i for i in range(1, amount) if given[i] < bound]
        whole, budget = sum([weights[i] for i in movable]), rest
        for i in movable:
            extra = min(bound - given[i], max(1, budget * weights[i] // whole), rest)
            given[i] = given[i] + extra
            rest = rest - extra
    return np.array(given)


def scatter_about(own_key, shape, deviation, most, shards=(), held_as=jnp.bfloat16):
    loudness = block_scale(own_key, shape, shards, -0.22, 0.18) if shards else 1.0
    drawn = jax.random.normal(own_key, shape, jnp.float32) * deviation * loudness
    return jnp.minimum(jnp.maximum(drawn, -most), most).astype(held_as)


def setup_inputs(seed: int = 0) -> dict:
    seeds = jax.random.split(jax.random.key(seed), 11)
    tokens = scatter_about(seeds[0], (TOKENS, D), 1.0, 6.0, ((0, 8), (1, 4)))
    norm_gain = jnp.clip(1.0 + 0.18 * jax.random.normal(seeds[1], (D,), jnp.float32), 0.1, 1.9)
    expert_ids_keys = jax.random.split(jax.random.fold_in(seeds[2], 1), TOKENS // TOK_DEV)
    expert_ids_turns = jax.random.permutation(jax.random.fold_in(seeds[2], 3), TOKENS // TOK_DEV)
    expert_ids = jax.vmap(lambda own, number: routed_block(jax.random.fold_in(seeds[2], 2), own, number, TOK_DEV, EXPERTS, TOP, CAP, 2))(expert_ids_keys, expert_ids_turns).reshape((TOKENS, TOP))
    expert_gates = jnp.clip(jnp.exp(math.log(1.0) - 1.609438 * jax.random.uniform(seeds[3], (TOKENS, TOP), jnp.float32) ** block_scale(seeds[3], (TOKENS, TOP), ((0, 8),), -0.2, 0.2)), 0.2, 1.0)
    gate_proj = scatter_about(seeds[4], (EXPERTS, D, EXPERT_DIM), D ** -0.5, 0.09375, ((0, 8), (2, 4)))
    up_proj = scatter_about(seeds[5], (EXPERTS, D, EXPERT_DIM), D ** -0.5, 0.09375, ((0, 8), (2, 4)))
    down_proj = scatter_about(seeds[6], (EXPERTS, EXPERT_DIM, D), EXPERT_DIM ** -0.5, 0.25, ((0, 8), (2, 4)))
    shared_gate = scatter_about(seeds[7], (D, SHARED), D ** -0.5, 0.09375, ((0, 8), (1, 4)))
    shared_up = scatter_about(seeds[8], (D, SHARED), D ** -0.5, 0.09375, ((0, 8), (1, 4)))
    shared_down = scatter_about(seeds[9], (SHARED, D), SHARED ** -0.5, 0.25, ((1, 4),))
    return dict(tokens=tokens, norm_gain=norm_gain, expert_ids=expert_ids, expert_gates=expert_gates, gate_proj=gate_proj, up_proj=up_proj, down_proj=down_proj, shared_gate=shared_gate, shared_up=shared_up, shared_down=shared_down)


def reference(tokens, norm_gain, expert_ids, expert_gates, gate_proj, up_proj, down_proj, shared_gate, shared_up, shared_down):
    floats = tokens.astype(jnp.float32)
    scale = lax.rsqrt(lax.optimization_barrier(jnp.mean(floats * floats, axis=-1, keepdims=True)) + 1e-06)
    normed = (floats * scale * norm_gain[None, :]).astype(jnp.bfloat16)
    shared_g = jnp.dot(normed, shared_gate, preferred_element_type=jnp.float32)
    shared_u = jnp.dot(normed, shared_up, preferred_element_type=jnp.float32)
    shared_hidden = (jax.nn.silu(shared_g) * shared_u).astype(jnp.bfloat16)
    shared_out = jnp.dot(shared_hidden, shared_down, preferred_element_type=jnp.float32)
    ids = expert_ids.reshape(N_EP, TOK_DEV * TOP)
    onehot = (ids[:, :, None] == jnp.arange(EXPERTS, dtype=jnp.int32)[None, None, :]).astype(jnp.int32)
    slots = lax.optimization_barrier(jnp.sum((jnp.cumsum(onehot, axis=1) - onehot) * onehot, axis=-1)).astype(jnp.int32)
    dest = (ids * CAP + slots).astype(jnp.int32)
    local_tok = jnp.repeat(jnp.arange(TOK_DEV, dtype=jnp.int32), TOP)
    glob = local_tok[None, :] + jnp.arange(N_EP, dtype=jnp.int32)[:, None] * TOK_DEV
    blocks = jnp.broadcast_to(jnp.arange(N_EP, dtype=jnp.int32)[:, None], dest.shape)
    owner = jnp.full((N_EP, EXPERTS * CAP), TOKENS, jnp.int32).at[blocks, dest].set(glob)
    weight = jnp.zeros((N_EP, EXPERTS * CAP), jnp.float32).at[blocks, dest].set(expert_gates.reshape(N_EP, TOK_DEV * TOP))
    owner = owner.reshape(N_EP, EXPERTS, CAP).transpose(1, 0, 2).reshape(EXPERTS, N_EP * CAP)
    weight = weight.reshape(N_EP, EXPERTS, CAP).transpose(1, 0, 2).reshape(EXPERTS, N_EP * CAP)
    padded = jnp.concatenate([normed, jnp.zeros((1, D), jnp.bfloat16)], axis=0)

    def step(total, item):
        rows_idx, rows_weight, w_gate, w_up, w_down = item
        rows = padded[rows_idx]
        g = jnp.dot(rows, w_gate, preferred_element_type=jnp.float32)
        u = jnp.dot(rows, w_up, preferred_element_type=jnp.float32)
        hidden = (jax.nn.silu(g) * u).astype(jnp.bfloat16)
        result = jnp.dot(hidden, w_down, preferred_element_type=jnp.float32).astype(jnp.bfloat16)
        return (total.at[rows_idx].add(rows_weight[:, None] * result.astype(jnp.float32)), None)
    total = jnp.zeros((TOKENS + 1, D), jnp.float32)
    total, _ = lax.scan(step, total, (owner, weight, gate_proj, up_proj, down_proj))
    return (total[:TOKENS] + shared_out).astype(jnp.bfloat16)
```

```python
import jax
import jax.numpy as jnp
from jax import lax
from jax.sharding import PartitionSpec as P

BF = jnp.bfloat16
F32 = jnp.float32


def swap(x, axis, mask):
    n = lax.axis_size(axis)
    return lax.ppermute(x, axis, [(d, d ^ mask) for d in range(n)])


def dot(a, b):
    return jnp.dot(a, b, preferred_element_type=F32)


def exchange(blocks, n_ep):
    if n_ep > 16:
        return lax.all_to_all(blocks, "ep", split_axis=0, concat_axis=0, tiled=True)
    return jnp.stack([blocks[0]] + [swap(blocks[k], "ep", k) for k in range(1, n_ep)])


def shards(
    tokens,
    norm_gain,
    expert_ids,
    expert_gates,
    gate_proj,
    up_proj,
    down_proj,
    shared_gate,
    shared_up,
    shared_down,
):
    n_ep = lax.axis_size("ep")
    n_tp = lax.axis_size("tp")
    ep = lax.axis_index("ep")
    tp = lax.axis_index("tp")
    half = n_tp // 2
    rows, quarter = tokens.shape
    width = quarter * n_tp
    top = expert_ids.shape[1]
    n_exp = gate_proj.shape[0] * n_ep
    cap = 3 * rows * top // (2 * n_exp)
    hid = gate_proj.shape[2]
    assert gate_proj.shape[0] == 1 and n_tp == 4

    def weights(q):
        def cut(w):
            return lax.dynamic_slice_in_dim(w[0], q * quarter, quarter, 0)

        gain = lax.dynamic_slice_in_dim(norm_gain, q * quarter, quarter, 0)[:, None]
        both = jnp.concatenate([cut(gate_proj), cut(up_proj)], axis=1).astype(F32)
        return (both * gain).astype(BF)

    hot = (expert_ids[:, :, None] == jnp.arange(n_exp, dtype=jnp.int32)).astype(F32)
    lower = (jnp.arange(rows)[:, None] > jnp.arange(rows)[None, :]).astype(BF)
    before = dot(lower, jnp.sum(hot, axis=1).astype(BF))
    slot = jnp.sum(hot * before[:, None, :], axis=-1).astype(jnp.int32)
    place = expert_ids ^ ep if n_ep <= 16 else expert_ids
    dest = place * cap + slot
    all_rows = n_exp * cap
    at = [dest[:, k : k + 1] == jnp.arange(all_rows, dtype=jnp.int32)[None, :] for k in range(top)]
    pick = sum(a.astype(F32) for a in at).astype(BF)
    mix = sum(jnp.where(a, expert_gates[:, k : k + 1], 0.0) for k, a in enumerate(at))
    mix_hi = lax.reduce_precision(mix, 8, 7)
    mix_lo = (mix - mix_hi).astype(BF)
    mix_hi = mix_hi.astype(BF)
    outgoing = lax.dot_general(
        pick, tokens, (((0,), (0,)), ((), ())), preferred_element_type=F32
    ).astype(BF)
    mine = exchange(outgoing.reshape(n_ep, cap, quarter), n_ep).reshape(all_rows, quarter)

    sent = jnp.concatenate([weights(tp ^ 2), weights(tp ^ 3)], axis=0)
    theirs_w = swap(sent, "tp", half)
    own_w0, own_w1 = weights(tp), weights(tp ^ 1)

    pair = jnp.stack([tokens, swap(tokens, "tp", 2)])
    whole = jnp.concatenate([pair, swap(pair, "tp", 1)], axis=0)
    squares = whole.astype(F32)
    scale = lax.rsqrt(jnp.sum(squares * squares, axis=(0, 2))[:, None] / width + 1e-06)

    share = jnp.concatenate([shared_gate, shared_up], axis=1)[None]
    blk = shared_gate.shape[0]
    order = [0]
    bit = n_ep // 2
    while bit:
        share = jnp.concatenate([share, swap(share, "ep", bit)], axis=0)
        order = order + [o ^ bit for o in order]
        bit //= 2

    other = swap(mine, "tp", 1)
    ms = mine.astype(F32)
    os_ = other.astype(F32)
    part_sq = jnp.sum(ms * ms, axis=-1) + jnp.sum(os_ * os_, axis=-1)
    row_sq = part_sq + swap(part_sq, "tp", half)
    row_scale = lax.rsqrt(row_sq / width + 1e-06)[:, None]
    part_own = dot(mine, own_w0) + dot(other, own_w1)
    part_their = dot(mine, theirs_w[:quarter]) + dot(other, theirs_w[quarter:])
    got = swap(jnp.concatenate([part_their, part_own], axis=1).astype(BF), "tp", half).astype(F32)
    full = (jnp.concatenate([part_own, part_their], axis=1) + got) * row_scale
    hidden = jnp.concatenate(
        [
            jax.nn.silu(full[:, :hid]) * full[:, hid : 2 * hid],
            jax.nn.silu(full[:, 2 * hid : 3 * hid]) * full[:, 3 * hid :],
        ],
        axis=1,
    ).astype(BF)
    hidden = jnp.concatenate([hidden, swap(hidden, "tp", 1)], axis=1)
    down = jnp.concatenate(
        [lax.dynamic_slice_in_dim(down_proj[0], (tp ^ r) * hid, hid, 0) for r in (0, 2, 1, 3)], axis=0
    )
    out = dot(hidden, down).astype(BF)
    back = exchange(out.reshape(n_ep, cap, quarter), n_ep).reshape(all_rows, quarter)

    acc = 0.0
    for k, o in enumerate(order):
        b = ep ^ o
        col = b * blk
        rel = (col // quarter) ^ tp
        pos = (rel & 1) * 2 + (rel >> 1)
        cut = lax.dynamic_slice(whole, (pos, 0, col % quarter), (1, rows, blk))[0].astype(F32)
        gain = lax.dynamic_slice_in_dim(norm_gain, col, blk, 0)[None, :]
        acc = acc + dot((cut * scale * gain).astype(BF), share[k])
    sh = shared_gate.shape[1]
    shared_hidden = (jax.nn.silu(acc[:, :sh]) * acc[:, sh:]).astype(BF)
    shared_out = dot(lax.all_gather(shared_hidden, "tp", axis=1, tiled=True), shared_down)

    routed = dot(mix_hi, back) + dot(mix_lo, back)
    return (routed + shared_out).astype(BF)


def solution(mesh):
    return jax.shard_map(
        shards,
        mesh=mesh,
        in_specs=(
            P("ep", "tp"),
            P(),
            P("ep", None),
            P("ep", None),
            P("ep", None, "tp"),
            P("ep", None, "tp"),
            P("ep", None, "tp"),
            P("ep", "tp"),
            P("ep", "tp"),
            P(None, "tp"),
        ),
        out_specs=P("ep", "tp"),
        check_vma=False,
    )
```

```python
import jax
import jax.numpy as jnp
from jax import lax
from jax.sharding import PartitionSpec as P

BF = jnp.bfloat16
F32 = jnp.float32


def swap(x, axis, mask):
    n = lax.axis_size(axis)
    return lax.ppermute(x, axis, [(d, d ^ mask) for d in range(n)])


def after(x, *deps):
    return lax.optimization_barrier((x,) + deps)[0]


def dot(a, b):
    return jnp.dot(a, b, preferred_element_type=F32)


def exchange(blocks, n_ep):
    if n_ep > 16:
        return lax.all_to_all(blocks, "ep", split_axis=0, concat_axis=0, tiled=True)
    got = {k: swap(blocks[k], "ep", k) for k in range(n_ep - 1, 0, -1)}
    return jnp.stack([blocks[0]] + [got[k] for k in range(1, n_ep)])


def shards(
    tokens,
    norm_gain,
    expert_ids,
    expert_gates,
    gate_proj,
    up_proj,
    down_proj,
    shared_gate,
    shared_up,
    shared_down,
):
    n_ep = lax.axis_size("ep")
    n_tp = lax.axis_size("tp")
    ep = lax.axis_index("ep")
    tp = lax.axis_index("tp")
    half = n_tp // 2
    rows, quarter = tokens.shape
    width = quarter * n_tp
    top = expert_ids.shape[1]
    n_exp = gate_proj.shape[0] * n_ep
    cap = 3 * rows * top // (2 * n_exp)
    hid = gate_proj.shape[2]
    assert gate_proj.shape[0] == 1 and n_tp == 4

    bits = [n_ep >> (i + 1) for i in range(n_ep.bit_length() - 1)]
    first = [swap(shared_gate, "ep", bits[0]), swap(shared_up, "ep", bits[0])]
    blk = shared_gate.shape[0]

    floats = tokens.astype(F32)
    sq = jnp.sum(floats * floats, axis=-1)[None, :]
    sq = sq + swap(sq, "tp", 1) + swap(sq, "tp", 2) + swap(sq, "tp", 3)
    scale = lax.rsqrt(sq[0] / width + 1e-06)[:, None]
    gain = lax.dynamic_slice_in_dim(norm_gain, tp * quarter, quarter, 0)[None, :]
    normed = (floats * scale * gain).astype(BF)

    hot = (expert_ids[:, :, None] == jnp.arange(n_exp, dtype=jnp.int32)).astype(F32)
    lower = (jnp.arange(rows)[:, None] > jnp.arange(rows)[None, :]).astype(BF)
    before = dot(lower, jnp.sum(hot, axis=1).astype(BF))
    slot = jnp.sum(hot * before[:, None, :], axis=-1).astype(jnp.int32)
    place = expert_ids ^ ep if n_ep <= 16 else expert_ids
    dest = place * cap + slot
    all_rows = n_exp * cap
    at = [dest[:, k : k + 1] == jnp.arange(all_rows, dtype=jnp.int32)[None, :] for k in range(top)]
    pick = sum(a.astype(F32) for a in at).astype(BF)
    mix = sum(jnp.where(a, expert_gates[:, k : k + 1], 0.0) for k, a in enumerate(at))
    mix_hi = lax.reduce_precision(mix, 8, 7)
    mix_lo = (mix - mix_hi).astype(BF)
    mix_hi = mix_hi.astype(BF)
    outgoing = lax.dot_general(
        pick, normed, (((0,), (0,)), ((), ())), preferred_element_type=F32
    ).astype(BF)
    gate_proj, up_proj, shared_gate, shared_up, _ = lax.optimization_barrier(
        (gate_proj, up_proj, shared_gate, shared_up, outgoing)
    )
    def half_of(y):
        def cut(w):
            return lax.dynamic_slice_in_dim(w[0], y * (2 * quarter), 2 * quarter, 0)

        return jnp.concatenate([cut(gate_proj), cut(up_proj)], axis=1)

    chip, core = tp // 2, tp % 2
    theirs_w = swap(half_of(1 - chip), "tp", half)
    own_w = half_of(chip)

    mine = exchange(outgoing.reshape(n_ep, cap, quarter), n_ep).reshape(all_rows, quarter)

    ours = after(normed, outgoing)
    over_y = swap(ours, "tp", 2)
    whole = jnp.concatenate([ours, over_y, swap(ours, "tp", 1), swap(over_y, "tp", 1)], axis=1)

    known = [0, bits[0]]
    blocks = jnp.concatenate(
        [jnp.concatenate([shared_gate, shared_up], axis=1), jnp.concatenate(first, axis=1)], axis=0
    )
    for bit in bits[1:-2]:
        blocks = jnp.concatenate([blocks, swap(blocks, "ep", bit)], axis=0)
        known = known + [k ^ bit for k in known]
    low, end = bits[-2:]
    blocks_low = swap(blocks, "ep", low)

    other = swap(mine, "tp", 1)

    def cut_w(w, c):
        return lax.dynamic_slice_in_dim(w, c * quarter, quarter, 0)

    part_own = dot(mine, cut_w(own_w, core)) + dot(other, cut_w(own_w, 1 - core))
    part_their = dot(mine, cut_w(theirs_w, core)) + dot(other, cut_w(theirs_w, 1 - core))
    parts = jnp.concatenate([part_their, part_own], axis=1).astype(BF)
    got = swap(parts, "tp", half).astype(F32)
    blocks_end = swap(blocks, "ep", end)
    blocks_last = swap(after(blocks_low, parts), "ep", end)
    full = jnp.concatenate([part_own, part_their], axis=1) + got
    hidden = jnp.concatenate(
        [
            jax.nn.silu(full[:, :hid]) * full[:, hid : 2 * hid],
            jax.nn.silu(full[:, 2 * hid : 3 * hid]) * full[:, 3 * hid :],
        ],
        axis=1,
    ).astype(BF)
    hidden = jnp.concatenate([hidden, swap(hidden, "tp", 1)], axis=1)
    down = jnp.concatenate(
        [lax.dynamic_slice_in_dim(down_proj[0], (tp ^ r) * hid, hid, 0) for r in (0, 2, 1, 3)], axis=0
    )
    out = dot(hidden, down).astype(BF)
    back = exchange(out.reshape(n_ep, cap, quarter), n_ep).reshape(all_rows, quarter)

    blocks_end, blocks_last, _ = lax.optimization_barrier((blocks_end, blocks_last, out))
    groups = ((0, blocks), (low, blocks_low), (end, blocks_end), (low ^ end, blocks_last))
    acc = 0.0
    pairs = [(k ^ g, w[i * blk : (i + 1) * blk]) for g, w in groups for i, k in enumerate(known)]
    for o, w in pairs:
        col = (ep ^ o) * blk
        rel = (col // quarter) ^ tp
        pos = (rel & 1) * 2 + (rel >> 1)
        cut = lax.dynamic_slice_in_dim(whole, pos * quarter + col % quarter, blk, 1)
        acc = acc + dot(cut, w)
    sh = shared_gate.shape[1]
    shared_hidden = (jax.nn.silu(acc[:, :sh]) * acc[:, sh:]).astype(BF)
    shared_out = dot(lax.all_gather(shared_hidden, "tp", axis=1, tiled=True), shared_down)

    routed = dot(mix_hi, back) + dot(mix_lo, back)
    return (routed + shared_out).astype(BF)


def solution(mesh):
    return jax.shard_map(
        shards,
        mesh=mesh,
        in_specs=(
            P("ep", "tp"),
            P(),
            P("ep", None),
            P("ep", None),
            P("ep", None, "tp"),
            P("ep", None, "tp"),
            P("ep", None, "tp"),
            P("ep", "tp"),
            P("ep", "tp"),
            P(None, "tp"),
        ),
        out_specs=P("ep", "tp"),
        check_vma=False,
    )
```
